256 devices in a mesh: sp: 64 (over z, y, core), tp: 4 (over x).
Axes of the slice: x: 4, y: 4, z: 8, core: 2. Of those that a mesh axis runs over, the one named last changes fastest.
Arguments:
- stream_in: bfloat16 [16384, 2048], P(('sp', 'tp')), may hold values from -6 to 6
- queries_one: bfloat16 [16384, 1024], P('sp', 'tp'), may hold values from -120 to 120
- queries_two: bfloat16 [16384, 1024], P('sp', 'tp'), may hold values from -120 to 120
- keys_one: bfloat16 [16384, 512], P('sp', 'tp'), may hold values from -7 to 7
- keys_two: bfloat16 [16384, 512], P('sp', 'tp'), may hold values from -7 to 7
- values: bfloat16 [16384, 1024], P('sp', 'tp'), may hold values from -6 to 6
- lambdas: float32 [8], P('tp'), may hold values from 0.3 to 0.8
- head_gain: float32 [256], replicated, may hold values from 0.1 to 1.9
- out_weight: bfloat16 [2048, 2048], P('tp'), may hold values from -0.125 to 0.125
- norm_gain: float32 [2048], replicated, may hold values from 0.1 to 1.9
- expert_ids: int32 [16384, 2], P(('sp', 'tp')), may hold values from 0 to 63, all different within a row; in each aligned block of 64 rows (0 to 63, 64 to 127, ...) at most 4 rows name the same one
- route_weight: float32 [16384, 2], P(('sp', 'tp')), may hold values from 0.1 to 1
- gate_weight: bfloat16 [64, 2048, 1024], P('sp', None, 'tp'), may hold values from -0.125 to 0.125
- up_weight: bfloat16 [64, 2048, 1024], P('sp', None, 'tp'), may hold values from -0.125 to 0.125
- down_weight: bfloat16 [64, 1024, 2048], P('sp', 'tp'), may hold values from -0.1875 to 0.1875
Outputs:
- mixed: bfloat16 [16384, 2048], P(('sp', 'tp'))
The draws below stay inside these ranges and needn't reach their ends.
Inputs may be any that keep to these rules, and one draw needn't show every extreme that they name: `expert_ids`: each row names 2 different experts. In each aligned block of 64 rows no expert is named more than 4 times, a bound that some block reaches.
All inputs are finite; a program needn't handle non-finite values.
Results may differ from the reference program's by a relative error of at most 0.013.
Values may be sent and summed in bfloat16 or wider, within the bound.
No kernel may reach another device: no remote copies, remote signals or barrier semaphores. Data moves between devices by JAX's collectives and lax.ppermute only.
A program may use at most 128 MiB of HBM per device.

```python
import math
import jax
import jax.numpy as jnp
import numpy as np
from jax import lax

D = 2048
HEADS = 8
KV_HEADS = 4
HEAD_DIM = 128
VAL_DIM = 256
EXPERT_FF = 1024
TOPK = 2
TOKENS = 16384
ROWS_DEV = 64
EXPERTS = 64
CAP = 4
N_SP = 64
N_TP = 4


def attention_draw(key):
    keys_first = jnp.clip(jax.random.normal(jax.random.fold_in(key, 11), (TOKENS, KV_HEADS * HEAD_DIM), jnp.float32) * 1.2, -7.0, 7.0)
    keys_second = jnp.clip(jax.random.normal(jax.random.fold_in(key, 12), (TOKENS, KV_HEADS * HEAD_DIM), jnp.float32) * 1.2, -7.0, 7.0)
    query_first = jnp.clip(jax.random.normal(jax.random.fold_in(key, 13), (TOKENS, HEADS * HEAD_DIM), jnp.float32) * 1.5, -9.0, 9.0)
    query_second = jnp.clip(jax.random.normal(jax.random.fold_in(key, 14), (TOKENS, HEADS * HEAD_DIM), jnp.float32) * 1.5, -9.0, 9.0)
    return (query_first, query_second, keys_first, keys_second)


def draw_queries_one(key, part):
    return attention_draw(key)[0].astype(jnp.bfloat16)


def draw_queries_two(key, part):
    return attention_draw(key)[1].astype(jnp.bfloat16)


def draw_keys_one(key, part):
    return attention_draw(key)[2].astype(jnp.bfloat16)


def draw_keys_two(key, part):
    return attention_draw(key)[3].astype(jnp.bfloat16)


def steps_of(key, dims, pieces, low, top_value):
    def one(position, blocks):
        heights = jax.random.uniform(jax.random.fold_in(jax.random.fold_in(key, 6), position), (blocks,), jnp.float32, low / len(pieces), top_value / len(pieces))
        return jnp.repeat(jnp.exp(heights), dims[position] // blocks).reshape((-1,) + (1,) * (len(dims) - position - 1))

    gain = one(*pieces[0])
    for cut in pieces[1:]:
        gain = gain * one(*cut)
    return gain


def deal_out(stream_key, own, number, rows, number_of, top, limit, lean):
    ranking = jax.random.permutation(stream_key, number_of)
    crowded, ordinary = shares(number_of, rows * top, limit, lean, True), shares(number_of, rows * top, limit, lean, False)
    places = jnp.arange(number_of)

    def named(lengths, turn):
        used = int((lengths > 0).sum())
        fixed = max(1, used // 4)
        shifted = fixed + (places - fixed + turn * (used - fixed)) % max(1, number_of - fixed)
        return jnp.zeros((number_of,), jnp.int32).at[ranking[jnp.where(places < fixed, places, shifted)]].set(jnp.asarray(lengths, jnp.int32))

    lengths = jnp.where(number % 4 == 0, named(crowded, number // 4), named(ordinary, number - number // 4 - 1))
    mixed = jax.random.permutation(jax.random.fold_in(own, 3), number_of)
    giver, receiver = mixed[0:number_of // 2 * 2:2], mixed[1:number_of // 2 * 2:2]
    room = jnp.minimum(lengths[giver] - 1, limit - lengths[receiver]) // 2
    room = jnp.where((giver == ranking[0]) | (receiver == ranking[0]) | (lengths[receiver] == 0), 0, jnp.maximum(room, 0))
    shifted = jax.random.randint(jax.random.fold_in(own, 4), (number_of // 2,), 0, 1 << 20) % (room + 1)
    lengths = lengths.at[giver].add(-shifted).at[receiver].add(shifted)
    labels = jnp.searchsorted(jnp.cumsum(lengths), jnp.arange(rows * top), side="right").astype(jnp.int32)
    listing = labels.reshape(top, rows).T
    listing = listing[jax.random.permutation(jax.random.fold_in(own, 1), rows)]
    turn = jax.random.randint(jax.random.fold_in(own, 2), (rows, 1), 0, top)
    return jnp.take_along_axis(listing, (jnp.arange(top)[None, :] + turn) % top, axis=1)


def shares(count, total, limit, slope, full):
    loads = [(1 << 20) // math.isqrt(grade ** slope) + 1 for grade in range(1, count + 1)]
    largest = limit if full else min(limit, max(-(-total // count), total * loads[0] // sum(loads)))
    least = 1 if total - largest >= count - 1 else 0
    given, rest = [largest] + [least] * (count - 1), total - largest - least * (count - 1)
    while rest > 0:
        free = [i for i in range(1, count) if given[i] < largest] or [i for i in range(1, count) if given[i] < limit]
        whole, left = sum([loads[i] for i in free]), rest
        for i in free:
            more = min(limit - given[i], max(1, left * loads[i] // whole), rest)
            given[i] = given[i] + more
            rest = rest - more
    return np.array(given)


def gaussian(stream_key, extent, width, bound, split=(), kind=jnp.bfloat16):
    entries = jax.random.normal(stream_key, extent, jnp.float32) * width
    if len(split) > 0:
        entries = steps_of(stream_key, extent, split, -0.22, 0.18) * entries
    return jnp.clip(entries, min=-bound, max=bound).astype(kind)


def setup_inputs(seed: int = 0) -> dict:
    seeds = jax.random.split(jax.random.key(seed), 16)
    stream_in = gaussian(seeds[0], (TOKENS, D), 1.0, 6.0, ((0, 256),))
    queries_one = draw_queries_one(jax.random.fold_in(seeds[15], 71), 0)
    queries_two = draw_queries_two(jax.random.fold_in(seeds[15], 71), 0)
    keys_one = draw_keys_one(jax.random.fold_in(seeds[15], 71), 0)
    keys_two = draw_keys_two(jax.random.fold_in(seeds[15], 71), 0)
    values = gaussian(seeds[5], (TOKENS, KV_HEADS * VAL_DIM), 1.0, 6.0, ((0, 64), (1, 4)))
    lambdas = jnp.clip(0.3 + 0.5 * jax.random.uniform(seeds[6], (HEADS,), jnp.float32) ** steps_of(seeds[6], (HEADS,), ((0, 4),), -0.2, 0.2), 0.3, 0.8)
    head_gain = jnp.clip(1.0 + 0.18 * jax.random.normal(seeds[7], (VAL_DIM,), jnp.float32), 0.1, 1.9)
    out_weight = gaussian(seeds[8], (HEADS * VAL_DIM, D), (HEADS * VAL_DIM) ** -0.5, 0.125, ((0, 4),))
    norm_gain = jnp.clip(1.0 + 0.18 * jax.random.normal(seeds[9], (D,), jnp.float32), 0.1, 1.9)
    expert_ids_keys = jax.random.split(jax.random.fold_in(seeds[10], 1), TOKENS // ROWS_DEV)
    expert_ids_turns = jax.random.permutation(jax.random.fold_in(seeds[10], 3), TOKENS // ROWS_DEV)
    expert_ids = jax.vmap(lambda own, number: deal_out(jax.random.fold_in(seeds[10], 2), own, number, ROWS_DEV, EXPERTS, TOPK, CAP, 1))(expert_ids_keys, expert_ids_turns).reshape((TOKENS, TOPK))
    route_weight = jnp.clip(0.1 + 0.9 * jax.random.uniform(seeds[11], (TOKENS, TOPK), jnp.float32) ** steps_of(seeds[11], (TOKENS, TOPK), ((0, 256),), -0.2, 0.2), 0.1, 1.0)
    gate_weight = gaussian(seeds[12], (EXPERTS, D, EXPERT_FF), D ** -0.5, 0.125, ((0, 64), (2, 4)))
    up_weight = gaussian(seeds[13], (EXPERTS, D, EXPERT_FF), D ** -0.5, 0.125, ((0, 64), (2, 4)))
    down_weight = gaussian(seeds[14], (EXPERTS, EXPERT_FF, D), EXPERT_FF ** -0.5, 0.1875, ((0, 64), (1, 4)))
    return {"stream_in": stream_in, "queries_one": queries_one, "queries_two": queries_two, "keys_one": keys_one, "keys_two": keys_two, "values": values, "lambdas": lambdas, "head_gain": head_gain, "out_weight": out_weight, "norm_gain": norm_gain, "expert_ids": expert_ids, "route_weight": route_weight, "gate_weight": gate_weight, "up_weight": up_weight, "down_weight": down_weight}


EPS = 1e-06
OUT_SCALE = 0.8

def mix_map(queries, keys, vals, allowed):
    scores = jnp.einsum('qrd,kd->rqk', queries, keys) * HEAD_DIM ** (-0.5)
    scores = jnp.where(allowed[None], scores, -jnp.inf)
    row_max = lax.optimization_barrier(jnp.max(scores, axis=-1, keepdims=True))
    exp_terms = jnp.exp(scores - row_max)
    totals = lax.optimization_barrier(jnp.sum(exp_terms, axis=-1, keepdims=True))
    weights = lax.optimization_barrier(exp_terms.astype(jnp.bfloat16)).astype(jnp.float32)
    return jnp.einsum('rqk,kv->rqv', weights, vals) / totals

def reference(stream_in, queries_one, queries_two, keys_one, keys_two, values, lambdas, head_gain, out_weight, norm_gain, expert_ids, route_weight, gate_weight, up_weight, down_weight):
    per_kv = HEADS // KV_HEADS
    q_block = math.gcd(TOKENS, 512)
    num_blocks = TOKENS // q_block
    key_pos = jnp.arange(TOKENS, dtype=jnp.int32)
    keys_first = keys_one.astype(jnp.float32)
    keys_second = keys_two.astype(jnp.float32)
    vals_all = values.astype(jnp.float32)

    def one_block(block_index):
        first_row = (block_index * q_block).astype(jnp.int32)
        q_first = lax.dynamic_slice_in_dim(queries_one, first_row, q_block, 0).astype(jnp.float32).reshape(q_block, HEADS, HEAD_DIM)
        q_second = lax.dynamic_slice_in_dim(queries_two, first_row, q_block, 0).astype(jnp.float32).reshape(q_block, HEADS, HEAD_DIM)
        query_pos = first_row + jnp.arange(q_block, dtype=jnp.int32)
        allowed = key_pos[None, :] <= query_pos[:, None]
        head_outs = []
        for kv_index in range(KV_HEADS):
            lo_head = kv_index * per_kv
            key_cols = slice(kv_index * HEAD_DIM, (kv_index + 1) * HEAD_DIM)
            val_cols = slice(kv_index * VAL_DIM, (kv_index + 1) * VAL_DIM)
            mix_first = mix_map(q_first[:, lo_head:lo_head + per_kv], keys_first[:, key_cols], vals_all[:, val_cols], allowed)
            mix_second = mix_map(q_second[:, lo_head:lo_head + per_kv], keys_second[:, key_cols], vals_all[:, val_cols], allowed)
            lambda_rows = lambdas[lo_head:lo_head + per_kv][:, None, None]
            head_outs.append(mix_first - lambda_rows * mix_second)
        difference = jnp.concatenate(head_outs, 0)
        mean_sq = lax.optimization_barrier(jnp.mean(difference * difference, axis=-1, keepdims=True))
        normed_heads = difference * lax.rsqrt(mean_sq + EPS) * head_gain * OUT_SCALE
        return normed_heads.transpose(1, 0, 2).reshape(q_block, HEADS * VAL_DIM).astype(jnp.bfloat16)
    heads_out = lax.map(one_block, jnp.arange(num_blocks, dtype=jnp.int32)).reshape(TOKENS, HEADS * VAL_DIM)
    col_width = HEADS * VAL_DIM // N_TP
    stream = stream_in.astype(jnp.float32)
    for group_no in range(N_TP):
        cols = slice(group_no * col_width, (group_no + 1) * col_width)
        partial_value = jnp.dot(heads_out[:, cols], out_weight[cols], preferred_element_type=jnp.float32)
        stream = stream + lax.optimization_barrier(partial_value.astype(jnp.bfloat16)).astype(jnp.float32)
    normed = (stream * lax.rsqrt(lax.optimization_barrier(jnp.mean(stream * stream, axis=-1, keepdims=True)) + EPS) * norm_gain).astype(jnp.bfloat16)
    flat_ids = expert_ids.reshape(-1)
    owners = jnp.arange(TOKENS * TOPK, dtype=jnp.int32) // TOPK
    rows_all = jnp.take(normed, owners, axis=0)
    capacity = N_SP * N_TP * CAP
    quarter = EXPERT_FF // N_TP

    def per_expert(collected, weights_item):
        gate_w, up_w, down_w, number = weights_item
        chosen = flat_ids == number
        places = jnp.cumsum(chosen.astype(jnp.int32)) - 1
        target = jnp.where(chosen, places, capacity).astype(jnp.int32)
        buffer = jnp.zeros((capacity + 1, D), jnp.bfloat16).at[target].set(rows_all)[:capacity]
        gate = jnp.dot(buffer, gate_w, preferred_element_type=jnp.float32)
        upper = jnp.dot(buffer, up_w, preferred_element_type=jnp.float32)
        hidden = (jax.nn.silu(gate) * upper).astype(jnp.bfloat16)
        summed = jnp.zeros((capacity, D), jnp.float32)
        for group_no in range(N_TP):
            units = slice(group_no * quarter, (group_no + 1) * quarter)
            partial_value = jnp.dot(hidden[:, units], down_w[units], preferred_element_type=jnp.float32)
            summed = summed + lax.optimization_barrier(partial_value.astype(jnp.bfloat16)).astype(jnp.float32)
        result = jnp.concatenate([summed.astype(jnp.bfloat16), jnp.zeros((1, D), jnp.bfloat16)], 0)
        collected = jnp.where(chosen[:, None], jnp.take(result, target, axis=0), collected)
        return (collected, None)
    collected, _ = lax.scan(per_expert, jnp.zeros((TOKENS * TOPK, D), jnp.bfloat16), (gate_weight, up_weight, down_weight, jnp.arange(EXPERTS, dtype=jnp.int32)))
    routed = lax.optimization_barrier(jnp.sum(collected.reshape(TOKENS, TOPK, D).astype(jnp.float32) * route_weight[:, :, None], axis=1))
    return (stream + routed).astype(jnp.bfloat16)
```

```python
import functools
import math

import jax
import jax.numpy as jnp
from jax import lax
from jax.experimental import pallas as pl
from jax.experimental.pallas import tpu as pltpu
from jax.sharding import Mesh
from jax.sharding import PartitionSpec as P


HEAD_DIM = 128
VAL_DIM = 256
LANES = 128

EPS = 1e-06
OUT_SCALE = 0.8
LOW = -1e30
EXP2_SCALE = HEAD_DIM ** (-0.5) * math.log2(math.e)

PARTS = 2
KEY_STEP = 512
CHAIN_ROWS = 512


def lanes_to(x, width):
    return jnp.concatenate([x] * (width // LANES), axis=1)


def attend_kernel(first, last, rows, part, part_rows, key_step, *refs):
    info, q_one_own, q_one_other, q_two_own, q_two_other, kv = refs[:6]
    refs = refs[6:]
    if not first:
        acc_in, max_in, sum_in = refs[:3]
        refs = refs[3:]
    if last:
        own_acc, own_stats, other_acc, other_stats, q_all, acc, row_max, row_sum = refs
    else:
        acc, row_max, row_sum, q_all = refs
    chip = info[0]
    core = info[1]
    step = pl.program_id(0)
    group = key_step // part_rows
    last_step = chip // group
    map_rows = 4 * rows

    @pl.when(step == 0)
    def _():
        for a, pieces in enumerate(((q_one_own, q_one_other), (q_two_own, q_two_other))):
            for h in range(2):
                for t in range(2):
                    start = a * map_rows + (2 * h + t) * rows
                    q_all[start : start + rows, :] = pieces[t][:, h * HEAD_DIM : (h + 1) * HEAD_DIM]
        if first:
            acc[...] = jnp.zeros_like(acc)
            row_max[...] = jnp.full(row_max.shape, LOW, jnp.float32)
            row_sum[...] = jnp.zeros_like(row_sum)
        else:
            acc[...] = acc_in[...]
            row_max[...] = max_in[...]
            row_sum[...] = sum_in[...]

    chain = min(CHAIN_ROWS, map_rows)

    def fold(a, start, masked):
        at = pl.ds(start, chain)
        keys = kv[:, a * HEAD_DIM : (a + 1) * HEAD_DIM]
        scores = lax.dot_general(
            q_all[at, :], keys, (((1,), (1,)), ((), ())), preferred_element_type=jnp.float32
        )
        if masked:
            row = lax.broadcasted_iota(jnp.int32, (chain, 1), 0) + start
            piece = (row // rows) % 2
            query = (2 * chip + jnp.where(piece == 0, core, 1 - core)) * rows + row % rows
            col = lax.broadcasted_iota(jnp.int32, (1, key_step), 1)
            holder = step * group + col // part_rows
            key = (2 * holder + core) * rows + part * part_rows + col % part_rows
            scores = jnp.where(key <= query, scores, LOW)
        old_max = row_max[at, :]
        new_max = jnp.maximum(old_max, jnp.max(scores, axis=1, keepdims=True))
        terms = jnp.exp2(scores * EXP2_SCALE - lanes_to(new_max * EXP2_SCALE, key_step))
        rescale = jnp.exp2((old_max - new_max) * EXP2_SCALE)
        row_max[at, :] = new_max
        part_sum = terms[:, :LANES]
        for j in range(1, key_step // LANES):
            part_sum = part_sum + terms[:, j * LANES : (j + 1) * LANES]
        row_sum[at, :] = row_sum[at, :] * rescale + part_sum
        mixed = jnp.dot(
            terms.astype(jnp.bfloat16), kv[:, 2 * HEAD_DIM :], preferred_element_type=jnp.float32
        )
        acc[at, :] = acc[at, :] * lanes_to(rescale, VAL_DIM) + mixed

    @pl.when(step < last_step)
    def _():
        for start in range(0, 2 * map_rows, chain):
            fold(start // map_rows, start, False)

    @pl.when(step == last_step)
    def _():
        for a in range(2):

            def masked_chain(i, _):
                fold(a, pl.multiple_of(a * map_rows + i * chain, chain), True)
                return 0

            lax.fori_loop(0, map_rows // chain, masked_chain, 0)

    if last:

        @pl.when(step == pl.num_programs(0) - 1)
        def _():
            lane = lax.broadcasted_iota(jnp.int32, (rows, LANES), 1)
            for t, (acc_out, stats_out) in enumerate(
                ((own_acc, own_stats), (other_acc, other_stats))
            ):
                stats = jnp.zeros((rows, LANES), jnp.float32)
                for k in range(4):
                    start = (2 * k + t) * rows
                    at = slice(start, start + rows)
                    acc_out[k * rows : (k + 1) * rows, :] = acc[at, :].astype(acc_out.dtype)
                    total = jnp.sum(row_sum[at, :], axis=1, keepdims=True)
                    stats = jnp.where(lane == k, row_max[at, :], stats)
                    stats = jnp.where(lane == 4 + k, total, stats)
                stats_out[...] = stats


def attend(info, queries, kv, state, part, parts):
    first, last = state is None, part == parts - 1
    rows = queries[0].shape[0]
    part_rows = rows // parts
    key_step = min(KEY_STEP, kv.shape[0])
    group = key_step // part_rows
    steps = kv.shape[0] // key_step
    whole = lambda shape: pl.BlockSpec(shape, lambda i, info: (0,) * len(shape))
    state_shapes = [
        jax.ShapeDtypeStruct((8 * rows, VAL_DIM), jnp.float32),
        jax.ShapeDtypeStruct((8 * rows, LANES), jnp.float32),
        jax.ShapeDtypeStruct((8 * rows, LANES), jnp.float32),
    ]
    q_scratch = pltpu.VMEM((8 * rows, HEAD_DIM), jnp.bfloat16)
    if last:
        out_shape = [
            jax.ShapeDtypeStruct((4 * rows, VAL_DIM), jnp.float32),
            jax.ShapeDtypeStruct((rows, LANES), jnp.float32),
            jax.ShapeDtypeStruct((4 * rows, VAL_DIM), jnp.bfloat16),
            jax.ShapeDtypeStruct((rows, LANES), jnp.float32),
        ]
        scratch = [q_scratch] + [pltpu.VMEM(s.shape, s.dtype) for s in state_shapes]
    else:
        out_shape = state_shapes
        scratch = [q_scratch]
    operands = list(queries) + [kv] + ([] if first else list(state))
    in_specs = [whole(q.shape) for q in queries]
    in_specs.append(
        pl.BlockSpec((key_step, kv.shape[1]), lambda i, info: (jnp.minimum(i, info[0] // group), 0))
    )
    if not first:
        in_specs += [whole(s.shape) for s in state_shapes]
    pairs = 8 * rows * kv.shape[0]
    return pl.pallas_call(
        functools.partial(attend_kernel, first, last, rows, part, part_rows, key_step),
        out_shape=out_shape,
        grid_spec=pltpu.PrefetchScalarGridSpec(
            num_scalar_prefetch=1,
            grid=(steps,),
            in_specs=in_specs,
            out_specs=[whole(s.shape) for s in out_shape],
            scratch_shapes=scratch,
        ),
        compiler_params=pltpu.CompilerParams(
            dimension_semantics=("arbitrary",), vmem_limit_bytes=28 * 1024 * 1024
        ),
        cost_estimate=pl.CostEstimate(
            flops=2 * pairs * (HEAD_DIM + VAL_DIM), transcendentals=pairs, bytes_accessed=kv.size * 2
        ),
    )(info, *operands)


def project_kernel(
    rows, lambdas, gain, own_acc, own_stats, other_acc, other_stats, weight, out
):
    stats_a, stats_b = own_stats[...], other_stats[...]

    def mix(k):
        at = slice(k * rows, (k + 1) * rows)
        max_a, max_b = stats_a[:, k : k + 1], stats_b[:, k : k + 1]
        top = jnp.maximum(max_a, max_b)
        share_a = jnp.exp2((max_a - top) * EXP2_SCALE)
        share_b = jnp.exp2((max_b - top) * EXP2_SCALE)
        total = stats_a[:, 4 + k : 5 + k] * share_a + stats_b[:, 4 + k : 5 + k] * share_b
        mixed = own_acc[at, :] * share_a + other_acc[at, :].astype(jnp.float32) * share_b
        return mixed / total

    heads = []
    for h in range(2):
        difference = mix(h) - lambdas[h] * mix(2 + h)
        mean_sq = jnp.mean(difference * difference, axis=-1, keepdims=True)
        normed = difference * lax.rsqrt(mean_sq + EPS) * gain[...] * OUT_SCALE
        heads.append(normed.astype(jnp.bfloat16))
    heads_out = jnp.concatenate(heads, axis=1)
    out[...] = jnp.dot(heads_out, weight[...], preferred_element_type=jnp.float32).astype(
        jnp.bfloat16
    )


def project(lambdas, head_gain, own_acc, own_stats, other_acc, other_stats, out_weight):
    rows = own_stats.shape[0]
    vmem = pl.BlockSpec(memory_space=pltpu.VMEM)
    return pl.pallas_call(
        functools.partial(project_kernel, rows),
        out_shape=jax.ShapeDtypeStruct((rows, out_weight.shape[1]), jnp.bfloat16),
        in_specs=[pl.BlockSpec(memory_space=pltpu.SMEM)] + [vmem] * 6,
        out_specs=vmem,
        compiler_params=pltpu.CompilerParams(vmem_limit_bytes=32 * 1024 * 1024),
        cost_estimate=pl.CostEstimate(
            flops=2 * rows * out_weight.size, transcendentals=0, bytes_accessed=out_weight.size * 2
        ),
        name="project",
    )(lambdas, head_gain.reshape(1, -1), own_acc, own_stats, other_acc, other_stats, out_weight)


def dispatch_kernel(tiles, stream_in, gain, selector, stream_out, send):
    attended = tiles[0].astype(jnp.float32)
    for t in range(1, tiles.shape[0]):
        attended = attended + tiles[t].astype(jnp.float32)
    stream = stream_in[...].astype(jnp.float32) + attended
    stream_out[...] = stream
    mean_sq = jnp.mean(stream * stream, axis=-1, keepdims=True)
    normed = (stream * lax.rsqrt(mean_sq + EPS) * gain[...]).astype(jnp.bfloat16)
    send[...] = jnp.dot(selector[...], normed, preferred_element_type=jnp.float32).astype(
        jnp.bfloat16
    )


def dispatch(tiles, stream_in, norm_gain, selector):
    rows, width = stream_in.shape
    vmem = pl.BlockSpec(memory_space=pltpu.VMEM)
    return pl.pallas_call(
        dispatch_kernel,
        out_shape=[
            jax.ShapeDtypeStruct((rows, width), jnp.float32),
            jax.ShapeDtypeStruct((selector.shape[0], width), jnp.bfloat16),
        ],
        in_specs=[vmem] * 4,
        out_specs=[vmem] * 2,
        cost_estimate=pl.CostEstimate(
            flops=2 * selector.size * width, transcendentals=0, bytes_accessed=4 * tiles.size
        ),
        name="dispatch",
    )(tiles, stream_in, norm_gain.reshape(1, -1), selector)


def experts_kernel(rows_in, *refs):
    sources, (out, gate, up, down, sums, sems) = refs[:16], refs[16:]
    half = rows_in.shape[1] // 2
    copies = []
    for g in range(4):
        gate_from, up_low, up_high, down_from = sources[4 * g : 4 * g + 4]
        copies.append(
            [
                (gate_from, gate.at[g]),
                (up_low, up.at[g, :half, :]),
                (up_high, up.at[g, half:, :]),
                (down_from, down.at[g]),
            ]
        )
    started = []
    for group in copies:
        started.append([])
        for source, target in group:
            number = sum(map(len, started))
            copy = pltpu.make_async_copy(source, target, sems.at[number])
            copy.start()
            started[-1].append(copy)
    for g, group in enumerate(started):
        for copy in group[:-1]:
            copy.wait()
        picked = rows_in[...]
        gated = jnp.dot(picked, gate[g], preferred_element_type=jnp.float32)
        upper = jnp.dot(picked, up[g], preferred_element_type=jnp.float32)
        hidden = (gated / (1.0 + jnp.exp(-gated)) * upper).astype(jnp.bfloat16)
        group[-1].wait()
        piece = jnp.dot(hidden, down[g], preferred_element_type=jnp.float32)
        if g == 0:
            sums[...] = piece
        elif g < 3:
            sums[...] = sums[...] + piece
        else:
            out[...] = (sums[...] + piece).astype(jnp.bfloat16)


def experts(rows_in, weights):
    rows, width = rows_in.shape
    units = weights[0].shape[1]
    vmem = pl.BlockSpec(memory_space=pltpu.VMEM)
    return pl.pallas_call(
        experts_kernel,
        out_shape=jax.ShapeDtypeStruct((rows, width), jnp.bfloat16),
        in_specs=[vmem] + [pl.BlockSpec(memory_space=pl.ANY)] * 16,
        out_specs=vmem,
        scratch_shapes=[
            pltpu.VMEM((4, width, units), jnp.bfloat16),
            pltpu.VMEM((4, width, units), jnp.bfloat16),
            pltpu.VMEM((4, units, width), jnp.bfloat16),
            pltpu.VMEM((rows, width), jnp.float32),
            pltpu.SemaphoreType.DMA((16,)),
        ],
        compiler_params=pltpu.CompilerParams(vmem_limit_bytes=40 * 1024 * 1024),
        cost_estimate=pl.CostEstimate(
            flops=24 * rows * width * units, transcendentals=4 * rows * units, bytes_accessed=24 * width * units
        ),
        name="experts",
    )(rows_in, *weights)


def collect_kernel(returned, choice_one, choice_two, route_weight, stream, out):
    picked_one = jnp.dot(choice_one[...], returned[...], preferred_element_type=jnp.float32)
    picked_two = jnp.dot(choice_two[...], returned[...], preferred_element_type=jnp.float32)
    routed = picked_one * route_weight[:, 0:1] + picked_two * route_weight[:, 1:2]
    out[...] = (stream[...] + routed).astype(jnp.bfloat16)


def collect(returned, choice_one, choice_two, route_weight, stream):
    vmem = pl.BlockSpec(memory_space=pltpu.VMEM)
    return pl.pallas_call(
        collect_kernel,
        out_shape=jax.ShapeDtypeStruct(stream.shape, jnp.bfloat16),
        in_specs=[vmem] * 5,
        out_specs=vmem,
        cost_estimate=pl.CostEstimate(
            flops=4 * choice_one.size * stream.shape[1], transcendentals=0, bytes_accessed=2 * returned.size
        ),
        name="collect",
    )(returned, choice_one, choice_two, route_weight, stream)


def body(
    stream_in,
    queries_one,
    queries_two,
    keys_one,
    keys_two,
    values,
    lambdas,
    head_gain,
    out_weight,
    norm_gain,
    expert_ids,
    route_weight,
    gate_weight,
    up_weight,
    down_weight,
):
    rows_q = queries_one.shape[0]
    chip = lax.axis_index("chip")
    core = lax.axis_index("core")
    peers = lax.axis_size("tp")

    part_rows = rows_q // PARTS
    gathered = []
    for i in range(PARTS):
        at = slice(i * part_rows, (i + 1) * part_rows)
        packed = jnp.concatenate([keys_one[at], keys_two[at], values[at]], 1)
        gathered.append(lax.all_gather(packed, "chip", axis=0, tiled=True))
    swap = [(0, 1), (1, 0)]
    other_one = lax.ppermute(queries_one, "core", swap)
    other_two = lax.ppermute(queries_two, "core", swap)

    up_ring = [(i, (i + 1) % peers) for i in range(peers)]
    down_ring = [(i, (i - 1) % peers) for i in range(peers)]
    half = up_weight.shape[1] // 2
    own = [gate_weight[0], up_weight[0, :half], up_weight[0, half:], down_weight[0]]
    below = [lax.ppermute(w, "tp", up_ring) for w in own]
    above = [lax.ppermute(w, "tp", down_ring) for w in own]
    across = [lax.ppermute(w, "tp", up_ring) for w in below[:2]]
    across += [lax.ppermute(w, "tp", down_ring) for w in above[2:]]
    weights = [*own, *below, *above, *across]

    rows_here = stream_in.shape[0]
    top_count = expert_ids.shape[1]
    experts_all = lax.axis_size("chip") * lax.axis_size("core")
    slot_cap = 2 * top_count * rows_here // experts_all
    flat_ids = expert_ids.reshape(-1)
    one_hot = (flat_ids[:, None] == lax.iota(jnp.int32, experts_all)[None, :]).astype(jnp.int32)
    ranks = jnp.sum((jnp.cumsum(one_hot, axis=0) - 1) * one_hot, axis=1)
    slots = (flat_ids * slot_cap + ranks).reshape(rows_here, top_count)
    all_slots = lax.iota(jnp.int32, experts_all * slot_cap)
    choice_one = (slots[:, 0:1] == all_slots[None, :]).astype(jnp.bfloat16)
    choice_two = (slots[:, 1:2] == all_slots[None, :]).astype(jnp.bfloat16)
    selector = (choice_one + choice_two).T

    info = jnp.stack([chip, core]).astype(jnp.int32)
    info, choice_one, choice_two, selector = lax.optimization_barrier(
        (info, choice_one, choice_two, selector)
    )
    queries = (queries_one, other_one, queries_two, other_two)
    state = None
    for i in range(PARTS):
        state = attend(info, queries, gathered[i], state, i, PARTS)
    own_acc, own_stats, other_acc, other_stats = state
    from_acc = lax.ppermute(other_acc, "core", swap)
    from_stats = lax.ppermute(other_stats, "core", swap)
    partial_rows = project(
        lambdas, head_gain, own_acc, own_stats, from_acc, from_stats, out_weight
    )
    tiles = lax.all_to_all(
        partial_rows.reshape(peers, rows_here, -1), "tp", 0, 0, tiled=True
    )
    stream, send_rows = dispatch(tiles, stream_in, norm_gain, selector)
    received = lax.all_to_all(send_rows, ("chip", "core"), split_axis=0, concat_axis=0, tiled=True)
    results = experts(received, weights)
    returned = lax.all_to_all(results, ("chip", "core"), split_axis=0, concat_axis=0, tiled=True)
    return collect(returned, choice_one, choice_two, route_weight, stream)


def solution(mesh):
    sp, tp = mesh.devices.shape
    split = Mesh(mesh.devices.reshape(sp // 2, 2, tp), ("chip", "core", "tp"))
    sp_axes = ("chip", "core")
    everywhere = ("chip", "core", "tp")
    return jax.shard_map(
        body,
        mesh=split,
        in_specs=(
            P(everywhere, None),
            P(sp_axes, "tp"),
            P(sp_axes, "tp"),
            P(sp_axes, "tp"),
            P(sp_axes, "tp"),
            P(sp_axes, "tp"),
            P("tp"),
            P(),
            P("tp", None),
            P(),
            P(everywhere, None),
            P(everywhere, None),
            P(sp_axes, None, "tp"),
            P(sp_axes, None, "tp"),
            P(sp_axes, "tp", None),
        ),
        out_specs=P(everywhere, None),
        check_vma=False,
    )
```

```python
import functools
import math

import jax
import jax.numpy as jnp
from jax import lax
from jax.experimental import pallas as pl
from jax.experimental.pallas import tpu as pltpu
from jax.sharding import Mesh
from jax.sharding import PartitionSpec as P


SP_AXES = ("z", "y", "core")

HEAD_DIM = 128
VAL_DIM = 256
LANES = 128

EPS = 1e-06
OUT_SCALE = 0.8
LOW = -1e30
EXP2_SCALE = HEAD_DIM ** (-0.5) * math.log2(math.e)

CHAIN_ROWS = 512
KERNEL_VMEM = 12 * 1024 * 1024


def lanes_to(x, width):
    return jnp.concatenate([x] * (width // LANES), axis=1)


def fold_kernel(first, last, units, rows, pieces, place, flags, *refs):
    if first:
        queries, refs = refs[:pieces], refs[pieces:]
        own, partner, q_all, acc, row_max, row_sum = refs[:6]
        refs = refs[6:]
    else:
        q_all, refs = refs[0], refs[1:]
        pairs, refs = refs[:units], refs[units:]
        acc, row_max, row_sum = refs[3:6]
        refs = refs[6:]
    if last:
        stats_out, refs = refs[0], refs[1:]
    (held,) = refs
    piece_rows = 4 * rows
    keys_here = 2 * rows
    unroll = min(pieces, 2 if first else 4)
    if first:
        held[0, :rows] = own[...]
        held[0, rows:] = partner[...]
    else:
        for i in range(units):
            held[i] = pairs[i][...]
    if first:
        for t in range(pieces):
            for k in range(4):
                start = t * piece_rows + k * rows
                q_all[start : start + rows, :] = queries[t][:, k * HEAD_DIM : (k + 1) * HEAD_DIM]
        acc[...] = jnp.zeros_like(acc)
        row_max[...] = jnp.full(row_max.shape, LOW, jnp.float32)
        row_sum[...] = jnp.zeros_like(row_sum)

    def fold(i, t):
        for start in range(0, piece_rows, CHAIN_ROWS):
            a = start // (2 * rows)
            at = pl.ds(pl.multiple_of(t * piece_rows + start, CHAIN_ROWS), CHAIN_ROWS)
            keys = held[i, :, a * HEAD_DIM : (a + 1) * HEAD_DIM]
            scores = lax.dot_general(
                q_all[at, :], keys, (((1,), (1,)), ((), ())), preferred_element_type=jnp.float32
            )
            if first:
                y, core = place[0], place[1]
                row = (lax.broadcasted_iota(jnp.int32, (CHAIN_ROWS, 1), 0) + start) % rows
                source = y - t + jnp.where(t > y, pieces, 0)
                query = (2 * source + core) * rows + row
                col = lax.broadcasted_iota(jnp.int32, (1, keys_here), 1)
                holder = 2 * y + jnp.where(col < rows, core, 1 - core)
                scores = jnp.where(holder * rows + col % rows <= query, scores, LOW)
            old_max = row_max[at, :]
            new_max = jnp.maximum(old_max, jnp.max(scores, axis=1, keepdims=True))
            terms = jnp.exp2(scores * EXP2_SCALE - lanes_to(new_max * EXP2_SCALE, keys_here))
            rescale = jnp.exp2((old_max - new_max) * EXP2_SCALE)
            row_max[at, :] = new_max
            part_sum = terms[:, :LANES]
            for j in range(1, keys_here // LANES):
                part_sum = part_sum + terms[:, j * LANES : (j + 1) * LANES]
            row_sum[at, :] = row_sum[at, :] * rescale + part_sum
            mixed = jnp.dot(
                terms.astype(jnp.bfloat16),
                held[i, :, 2 * HEAD_DIM :],
                preferred_element_type=jnp.float32,
            )
            acc[at, :] = acc[at, :] * lanes_to(rescale, VAL_DIM) + mixed

    def unit(i, _):
        @pl.when(flags[i] > 0)
        def _():
            lax.fori_loop(0, pieces, lambda t, _: (fold(i, t), 0)[1], 0, unroll=unroll)

        return 0

    lax.fori_loop(0, units, unit, 0)

    if last:
        lane = lax.broadcasted_iota(jnp.int32, (rows, LANES), 1)
        stats = jnp.zeros((rows, LANES), jnp.float32)
        for t in range(pieces):
            for k in range(4):
                start = t * piece_rows + k * rows
                at = slice(start, start + rows)
                total = jnp.sum(row_sum[at, :], axis=1, keepdims=True)
                stats = jnp.where(lane == 8 * t + k, row_max[at, :], stats)
                stats = jnp.where(lane == 8 * t + 4 + k, total, stats)
        stats_out[...] = stats.T[: 8 * pieces, :]


def fold_planes(place, flags, queries, pairs, state, last, pieces):
    first = state is None
    units = len(pairs)
    keys_here, width = sum(x.shape[0] for x in pairs[0]), pairs[0][0].shape[1]
    rows = keys_here // 2
    chunks = [x for pair in pairs for x in pair]
    vmem = pl.BlockSpec(memory_space=pltpu.VMEM)
    smem = pl.BlockSpec(memory_space=pltpu.SMEM)
    all_rows = pieces * 4 * rows
    state_shapes = [
        jax.ShapeDtypeStruct((all_rows, VAL_DIM), jnp.float32),
        jax.ShapeDtypeStruct((all_rows, LANES), jnp.float32),
        jax.ShapeDtypeStruct((all_rows, LANES), jnp.float32),
    ]
    if first:
        operands = [place, flags, *queries, *chunks]
        out_shape = [jax.ShapeDtypeStruct((all_rows, HEAD_DIM), jnp.bfloat16), *state_shapes]
        aliases = {}
    else:
        operands = [place, flags, queries, *chunks, *state]
        out_shape = list(state_shapes)
        aliases = {3 + units + i: i for i in range(3)}
    if last:
        out_shape.append(jax.ShapeDtypeStruct((8 * pieces, rows), jnp.float32))
    terms = all_rows * keys_here * units
    return pl.pallas_call(
        functools.partial(fold_kernel, first, last, units, rows, pieces),
        out_shape=out_shape,
        in_specs=[smem, smem] + [vmem] * (len(operands) - 2),
        out_specs=[vmem] * len(out_shape),
        scratch_shapes=[pltpu.VMEM((units, keys_here, width), jnp.bfloat16)],
        input_output_aliases=aliases,
        compiler_params=pltpu.CompilerParams(vmem_limit_bytes=KERNEL_VMEM),
        cost_estimate=pl.CostEstimate(
            flops=2 * terms * (HEAD_DIM + VAL_DIM), transcendentals=terms, bytes_accessed=0
        ),
    )(*operands)


def difference_kernel(rows, pieces, lambdas, acc, *refs):
    stats, (own, *outs) = refs[:pieces], refs[pieces:]
    coefs = []
    for t in range(pieces):
        tiles = []
        for s in range(pieces):
            at = 8 * ((t - s) % pieces)
            tiles.append(stats[s][at : at + 8, :])
        top = functools.reduce(jnp.maximum, tiles)
        total = jnp.zeros_like(top)
        for s in range(pieces):
            share = jnp.exp2((tiles[s] - top) * EXP2_SCALE)
            if s == 0:
                own_share = share
            total = total + share * jnp.concatenate([tiles[s][4:], tiles[s][:4]], axis=0)
        coefs.append(own_share / total)
    coefs.append(jnp.zeros((LANES - 8 * pieces, rows), jnp.float32))
    coefs = jnp.concatenate(coefs, axis=0).T
    for t, out in enumerate((own, *outs)):
        for h in range(2):
            start = t * 4 * rows + h * rows
            one, two = 8 * t + h, 8 * t + 2 + h
            mix_one = acc[start : start + rows, :] * coefs[:, one : one + 1]
            start += 2 * rows
            mix_two = acc[start : start + rows, :] * coefs[:, two : two + 1]
            out[h * rows : (h + 1) * rows, :] = (mix_one - lambdas[h] * mix_two).astype(out.dtype)


def differences(lambdas, acc, stats):
    pieces = len(stats)
    rows = acc.shape[0] // (4 * pieces)
    vmem = pl.BlockSpec(memory_space=pltpu.VMEM)
    shape = (2 * rows, VAL_DIM)
    return pl.pallas_call(
        functools.partial(difference_kernel, rows, pieces),
        out_shape=[jax.ShapeDtypeStruct(shape, jnp.float32)]
        + [jax.ShapeDtypeStruct(shape, jnp.bfloat16)] * (pieces - 1),
        in_specs=[pl.BlockSpec(memory_space=pltpu.SMEM)] + [vmem] * (1 + pieces),
        out_specs=[vmem] * pieces,
        compiler_params=pltpu.CompilerParams(vmem_limit_bytes=KERNEL_VMEM),
        cost_estimate=pl.CostEstimate(
            flops=3 * acc.size, transcendentals=0, bytes_accessed=4 * acc.size
        ),
        name="differences",
    )(lambdas, acc, *stats)


def project_kernel(rows, gain, weight, own, *refs):
    shares, out = refs[:-1], refs[-1]
    heads = []
    for h in range(2):
        at = slice(h * rows, (h + 1) * rows)
        difference = own[at, :]
        for share in shares:
            difference = difference + share[at, :].astype(jnp.float32)
        mean_sq = jnp.mean(difference * difference, axis=-1, keepdims=True)
        normed = difference * lax.rsqrt(mean_sq + EPS) * gain[...] * OUT_SCALE
        heads.append(normed.astype(jnp.bfloat16))
    heads_out = jnp.concatenate(heads, axis=1)
    out[...] = jnp.dot(heads_out, weight[...], preferred_element_type=jnp.float32).astype(
        jnp.bfloat16
    )


def project(head_gain, out_weight, own, shares):
    rows = own.shape[0] // 2
    vmem = pl.BlockSpec(memory_space=pltpu.VMEM)
    return pl.pallas_call(
        functools.partial(project_kernel, rows),
        out_shape=jax.ShapeDtypeStruct((rows, out_weight.shape[1]), jnp.bfloat16),
        in_specs=[vmem] * (3 + len(shares)),
        out_specs=vmem,
        compiler_params=pltpu.CompilerParams(vmem_limit_bytes=KERNEL_VMEM),
        cost_estimate=pl.CostEstimate(
            flops=2 * rows * out_weight.size, transcendentals=0, bytes_accessed=out_weight.size * 2
        ),
        name="project",
    )(head_gain.reshape(1, -1), out_weight, own, *shares)


def run_copies(moves, sems):
    copies = [
        pltpu.make_async_copy(source, target, sems.at[i])
        for i, (source, target) in enumerate(moves)
    ]
    for copy in copies:
        copy.start()
    for copy in copies:
        copy.wait()


def pack_kernel(key_one, key_two, values, query_one, query_two, keys_out, queries_out, sems):
    d, width = HEAD_DIM, query_one.shape[1]
    run_copies(
        [
            (key_one, keys_out.at[:, :d]),
            (key_two, keys_out.at[:, d : 2 * d]),
            (values, keys_out.at[:, 2 * d :]),
            (query_one, queries_out.at[:, :width]),
            (query_two, queries_out.at[:, width:]),
        ],
        sems,
    )


def pack(keys_one, keys_two, values, queries_one, queries_two):
    rows = values.shape[0]
    vmem = pl.BlockSpec(memory_space=pltpu.VMEM)
    width = 2 * HEAD_DIM + VAL_DIM
    return pl.pallas_call(
        pack_kernel,
        out_shape=[jax.ShapeDtypeStruct((rows, width), jnp.bfloat16)] * 2,
        in_specs=[pl.BlockSpec(memory_space=pltpu.HBM)] * 5,
        out_specs=[vmem] * 2,
        scratch_shapes=[pltpu.SemaphoreType.DMA((5,))],
        compiler_params=pltpu.CompilerParams(vmem_limit_bytes=KERNEL_VMEM),
        name="pack",
    )(keys_one, keys_two, values, queries_one, queries_two)


def pack_weights_kernel(gate, up, down, low, high, sems):
    width, units = gate.shape[1:]
    half = width // 2
    moves = [
        (gate.at[0], low.at[:width]),
        (up.at[0, :half], low.at[width:]),
        (up.at[0, half:], high.at[:half]),
    ]
    for j in range(0, width, units):
        moves.append((down.at[0, :, j : j + units], high.at[half + j : half + j + units]))
    run_copies(moves, sems)


def pack_weights(gate, up, down):
    width, units = gate.shape[1:]
    hbm = pl.BlockSpec(memory_space=pltpu.HBM)
    return pl.pallas_call(
        pack_weights_kernel,
        out_shape=[jax.ShapeDtypeStruct((width + width // 2, units), gate.dtype)] * 2,
        in_specs=[hbm] * 3,
        out_specs=[hbm] * 2,
        scratch_shapes=[pltpu.SemaphoreType.DMA((3 + width // units,))],
        compiler_params=pltpu.CompilerParams(vmem_limit_bytes=KERNEL_VMEM),
        name="pack_weights",
    )(gate, up, down)


def places():
    planes = lax.axis_size("z")
    plane, y, core = lax.axis_index("z"), lax.axis_index("y"), lax.axis_index("core")
    half = planes // 2

    def held(d, from_below):
        return jnp.where(from_below, plane - d, plane + d - planes)

    flags = [jnp.stack([plane])]
    for d in range(1, half + 1):
        pairs = [held(d, core == 0) if d < half else plane - d]
        if d > 1:
            pairs.append(held(d - 1, core == 1))
        flags.append(jnp.stack(pairs))
    flags = [(flag >= 0).astype(jnp.int32) for flag in flags]
    return jnp.stack([y, core]).astype(jnp.int32), flags


def attend(place, flags, queries_one, queries_two, keys_one, keys_two, values, lambdas):
    planes, pieces = lax.axis_size("z"), lax.axis_size("y")
    swap = [(0, 1), (1, 0)]
    packed, both = pack(keys_one, keys_two, values, queries_one, queries_two)
    queries = [both]
    for t in range(1, pieces):
        queries.append(lax.ppermute(both, "y", [(i, (i + t) % pieces) for i in range(pieces)]))
    partner = lax.ppermute(packed, "core", swap)

    half = planes // 2
    received, swapped = [None], [None]
    for d in range(1, half + 1):
        moves = [((z - 1, 0), (z, 0)) for z in range(d, planes)]
        for first_plane in range(half):
            z = (first_plane - d) % planes
            moves.append((((z + 1) % planes, 1), (z, 1)))

        def along(x, flip):
            flat = [(2 * a + (b ^ flip), 2 * e + f) for (a, b), (e, f) in moves]
            return lax.ppermute(x, ("z", "core"), flat)

        if d == 1:
            received.append(jnp.concatenate([along(packed, 0), along(packed, 1)], 0))
        else:
            received.append(along(received[-1], 0))
        if d < half:
            swapped.append(lax.ppermute(received[-1], "core", swap))

    q_all, *state = fold_planes(place, flags[0], queries, [(packed, partner)], None, False, pieces)
    for d in range(1, half + 1):
        pairs = [(received[d],)]
        if d > 1:
            pairs.append((swapped[d - 1],))
        state = fold_planes(place, flags[d], q_all, pairs, state, d == half, pieces)
    acc, _, _, own_stats = state
    stats = [own_stats]
    for t in range(1, pieces):
        ring = [(i, (i + t) % pieces) for i in range(pieces)]
        stats.append(lax.ppermute(own_stats, "y", ring))
    own, *others = differences(lambdas, acc, stats)
    shares = []
    for t in range(1, pieces):
        ring = [(i, (i - t) % pieces) for i in range(pieces)]
        shares.append(lax.ppermute(others[t - 1], "y", ring))
    return own, shares


def dispatch_kernel(tiles, stream_in, gain, selector, stream_out, send):
    attended = tiles[0].astype(jnp.float32)
    for t in range(1, tiles.shape[0]):
        attended = attended + tiles[t].astype(jnp.float32)
    stream = stream_in[...].astype(jnp.float32) + attended
    stream_out[...] = stream
    mean_sq = jnp.mean(stream * stream, axis=-1, keepdims=True)
    normed = (stream * lax.rsqrt(mean_sq + EPS) * gain[...]).astype(jnp.bfloat16)
    send[...] = jnp.dot(selector[...], normed, preferred_element_type=jnp.float32).astype(
        jnp.bfloat16
    )


def dispatch(tiles, stream_in, norm_gain, selector):
    rows, width = stream_in.shape
    vmem = pl.BlockSpec(memory_space=pltpu.VMEM)
    return pl.pallas_call(
        dispatch_kernel,
        out_shape=[
            jax.ShapeDtypeStruct((rows, width), jnp.float32),
            jax.ShapeDtypeStruct((selector.shape[0], width), jnp.bfloat16),
        ],
        in_specs=[vmem] * 4,
        out_specs=[vmem] * 2,
        compiler_params=pltpu.CompilerParams(vmem_limit_bytes=KERNEL_VMEM),
        cost_estimate=pl.CostEstimate(
            flops=2 * selector.size * width, transcendentals=0, bytes_accessed=4 * tiles.size
        ),
        name="dispatch",
    )(tiles, stream_in, norm_gain.reshape(1, -1), selector)


def experts_kernel(rows_in, *refs):
    sources, (out, held, sums, sems) = refs[:8], refs[8:]
    width, units = rows_in.shape[1], held.shape[2]
    half = width // 2

    def moves(g, low, high):
        return [
            pltpu.make_async_copy(low, held.at[g, : width + half], sems.at[g, 0]),
            pltpu.make_async_copy(
                high.at[:half], held.at[g, width + half : 2 * width], sems.at[g, 1]
            ),
            pltpu.make_async_copy(high.at[half:], held.at[g, 2 * width :], sems.at[g, 2]),
        ]

    for g in range(4):
        for move in moves(g, *sources[2 * g : 2 * g + 2]):
            move.start()
    sums[...] = jnp.zeros_like(sums)

    def add_group(g, _):
        waits = moves(g, *sources[:2])
        waits[0].wait()
        waits[1].wait()
        picked = rows_in[...]
        gated = jnp.dot(picked, held[g, :width], preferred_element_type=jnp.float32)
        upper = jnp.dot(picked, held[g, width : 2 * width], preferred_element_type=jnp.float32)
        hidden = (gated / (1.0 + jnp.exp(-gated)) * upper).astype(jnp.bfloat16)
        waits[2].wait()
        for j in range(0, width, units):
            sums[:, j : j + units] += jnp.dot(
                hidden,
                held[g, 2 * width + j : 2 * width + j + units],
                preferred_element_type=jnp.float32,
            )
        return 0

    lax.fori_loop(0, 4, add_group, 0)
    out[...] = sums[...].astype(jnp.bfloat16)


def experts(rows_in, weights):
    rows, width = rows_in.shape
    units = weights[0].shape[1]
    vmem = pl.BlockSpec(memory_space=pltpu.VMEM)
    return pl.pallas_call(
        experts_kernel,
        out_shape=jax.ShapeDtypeStruct((rows, width), jnp.bfloat16),
        in_specs=[vmem] + [pl.BlockSpec(memory_space=pltpu.HBM)] * 8,
        out_specs=vmem,
        scratch_shapes=[
            pltpu.VMEM((4, 3 * width, units), jnp.bfloat16),
            pltpu.VMEM((rows, width), jnp.float32),
            pltpu.SemaphoreType.DMA((4, 3)),
        ],
        compiler_params=pltpu.CompilerParams(vmem_limit_bytes=24 * 1024 * 1024),
        cost_estimate=pl.CostEstimate(
            flops=24 * rows * width * units, transcendentals=4 * rows * units, bytes_accessed=24 * width * units
        ),
        name="experts",
    )(rows_in, *weights)


def collect_kernel(returned, choice_one, choice_two, route_weight, stream, out):
    picked_one = jnp.dot(choice_one[...], returned[...], preferred_element_type=jnp.float32)
    picked_two = jnp.dot(choice_two[...], returned[...], preferred_element_type=jnp.float32)
    routed = picked_one * route_weight[:, 0:1] + picked_two * route_weight[:, 1:2]
    out[...] = (stream[...] + routed).astype(jnp.bfloat16)


def collect(returned, choice_one, choice_two, route_weight, stream):
    vmem = pl.BlockSpec(memory_space=pltpu.VMEM)
    return pl.pallas_call(
        collect_kernel,
        out_shape=jax.ShapeDtypeStruct(stream.shape, jnp.bfloat16),
        in_specs=[vmem] * 5,
        out_specs=vmem,
        compiler_params=pltpu.CompilerParams(vmem_limit_bytes=KERNEL_VMEM),
        cost_estimate=pl.CostEstimate(
            flops=4 * choice_one.size * stream.shape[1], transcendentals=0, bytes_accessed=2 * returned.size
        ),
        name="collect",
    )(returned, choice_one, choice_two, route_weight, stream)


def body(
    stream_in,
    queries_one,
    queries_two,
    keys_one,
    keys_two,
    values,
    lambdas,
    head_gain,
    out_weight,
    norm_gain,
    expert_ids,
    route_weight,
    gate_weight,
    up_weight,
    down_weight,
):
    peers = lax.axis_size("tp")

    up_ring = [(i, (i + 1) % peers) for i in range(peers)]
    down_ring = [(i, (i - 1) % peers) for i in range(peers)]
    own_low, own_high = pack_weights(gate_weight, up_weight, down_weight)
    below = [lax.ppermute(w, "tp", up_ring) for w in (own_low, own_high)]
    above = [lax.ppermute(w, "tp", down_ring) for w in (own_low, own_high)]
    across = [lax.ppermute(below[0], "tp", up_ring), lax.ppermute(above[1], "tp", down_ring)]
    weights = [own_low, own_high, *below, *above, *across]

    rows_here = stream_in.shape[0]
    top_count = expert_ids.shape[1]
    experts_all = lax.axis_size(SP_AXES)
    slot_cap = 2 * top_count * rows_here // experts_all
    flat_ids = expert_ids.reshape(-1)
    one_hot = (flat_ids[:, None] == lax.iota(jnp.int32, experts_all)[None, :]).astype(jnp.int32)
    ranks = jnp.sum((jnp.cumsum(one_hot, axis=0) - 1) * one_hot, axis=1)
    slots = (flat_ids * slot_cap + ranks).reshape(rows_here, top_count)
    all_slots = lax.iota(jnp.int32, experts_all * slot_cap)
    choice_one = (slots[:, 0:1] == all_slots[None, :]).astype(jnp.bfloat16)
    choice_two = (slots[:, 1:2] == all_slots[None, :]).astype(jnp.bfloat16)
    selector = (choice_one + choice_two).T

    place, flags = places()
    place, flags, choice_one, choice_two, selector = lax.optimization_barrier(
        (place, flags, choice_one, choice_two, selector)
    )
    own, shares = attend(
        place, flags, queries_one, queries_two, keys_one, keys_two, values, lambdas
    )
    partial_rows = project(head_gain, out_weight, own, shares)
    tiles = lax.all_to_all(
        partial_rows.reshape(peers, rows_here, -1), "tp", 0, 0, tiled=True
    )
    stream, send_rows = dispatch(tiles, stream_in, norm_gain, selector)
    received = lax.all_to_all(
        send_rows, SP_AXES, split_axis=0, concat_axis=0, tiled=True
    )
    results = experts(received, weights)
    returned = lax.all_to_all(results, SP_AXES, split_axis=0, concat_axis=0, tiled=True)
    return collect(returned, choice_one, choice_two, route_weight, stream)


def solution(mesh):
    sp, tp = mesh.devices.shape
    planes = max(sp // 8, 2)
    split = Mesh(
        mesh.devices.reshape(planes, sp // (2 * planes), 2, tp), ("z", "y", "core", "tp")
    )
    everywhere = ("z", "y", "core", "tp")
    sp_axes = SP_AXES
    return jax.shard_map(
        body,
        mesh=split,
        in_specs=(
            P(everywhere, None),
            P(sp_axes, "tp"),
            P(sp_axes, "tp"),
            P(sp_axes, "tp"),
            P(sp_axes, "tp"),
            P(sp_axes, "tp"),
            P("tp"),
            P(),
            P("tp", None),
            P(),
            P(everywhere, None),
            P(everywhere, None),
            P(sp_axes, None, "tp"),
            P(sp_axes, None, "tp"),
            P(sp_axes, "tp", None),
        ),
        out_specs=P(everywhere, None),
        check_vma=False,
    )
```

```python
import functools
import math

import jax
import jax.numpy as jnp
from jax import lax
from jax.experimental import pallas as pl
from jax.experimental.pallas import tpu as pltpu
from jax.sharding import Mesh
from jax.sharding import PartitionSpec as P


SP_AXES = ("z", "y", "core")

HEAD_DIM = 128
VAL_DIM = 256
LANES = 128

EPS = 1e-06
OUT_SCALE = 0.8
LOW = -1e30
EXP2_SCALE = HEAD_DIM ** (-0.5) * math.log2(math.e)

CHAIN_ROWS = 512
KERNEL_VMEM = 12 * 1024 * 1024
PACK_VMEM = 65300000
EXPERTS_VMEM = 63300000
ALL_VMEM = 62800000


def lanes_to(x, width):
    return jnp.concatenate([x] * (width // LANES), axis=1)


def fold_kernel(first, units, rows, pieces, place, flags, *refs):
    if first:
        queries, refs = refs[:pieces], refs[pieces:]
        own, partner, below, q_all, acc, row_max, row_sum = refs[:7]
        refs = refs[7:]
    else:
        q_all, refs = refs[0], refs[1:]
        pairs, refs = refs[:units], refs[units:]
        acc, row_max, row_sum = refs[3:6]
        refs = refs[6:]
    (held,) = refs
    piece_rows = 4 * rows
    keys_here = 2 * rows
    unroll = min(pieces, 2 if first else 4)
    if first:
        held[0, :rows] = own[...]
        held[0, rows:] = partner[...]
        held[1] = below[...]
    else:
        for i in range(units):
            held[i] = pairs[i][...]
    if first:
        for t in range(pieces):
            for k in range(4):
                start = t * piece_rows + k * rows
                q_all[start : start + rows, :] = queries[t][:, k * HEAD_DIM : (k + 1) * HEAD_DIM]
        acc[...] = jnp.zeros_like(acc)
        row_max[...] = jnp.full(row_max.shape, LOW, jnp.float32)
        row_sum[...] = jnp.zeros_like(row_sum)

    def fold(i, t):
        for start in range(0, piece_rows, CHAIN_ROWS):
            a = start // (2 * rows)
            at = pl.ds(pl.multiple_of(t * piece_rows + start, CHAIN_ROWS), CHAIN_ROWS)
            keys = held[i, :, a * HEAD_DIM : (a + 1) * HEAD_DIM]
            scores = lax.dot_general(
                q_all[at, :], keys, (((1,), (1,)), ((), ())), preferred_element_type=jnp.float32
            )
            if first:
                y, core = place[0], place[1]
                row = (lax.broadcasted_iota(jnp.int32, (CHAIN_ROWS, 1), 0) + start) % rows
                source = y - t + jnp.where(t > y, pieces, 0)
                query = (2 * source + core) * rows + row
                col = lax.broadcasted_iota(jnp.int32, (1, keys_here), 1)
                holder = 2 * y + jnp.where(col < rows, core, 1 - core)
                last_key = query + i * (2 * pieces * rows)
                scores = jnp.where(holder * rows + col % rows <= last_key, scores, LOW)
            old_max = row_max[at, :]
            new_max = jnp.maximum(old_max, jnp.max(scores, axis=1, keepdims=True))
            terms = jnp.exp2(scores * EXP2_SCALE - lanes_to(new_max * EXP2_SCALE, keys_here))
            rescale = jnp.exp2((old_max - new_max) * EXP2_SCALE)
            row_max[at, :] = new_max
            part_sum = terms[:, :LANES]
            for j in range(1, keys_here // LANES):
                part_sum = part_sum + terms[:, j * LANES : (j + 1) * LANES]
            row_sum[at, :] = row_sum[at, :] * rescale + part_sum
            mixed = jnp.dot(
                terms.astype(jnp.bfloat16),
                held[i, :, 2 * HEAD_DIM :],
                preferred_element_type=jnp.float32,
            )
            acc[at, :] = acc[at, :] * lanes_to(rescale, VAL_DIM) + mixed

    def unit(i, _):
        @pl.when(flags[i] > 0)
        def _():
            lax.fori_loop(0, pieces, lambda t, _: (fold(i, t), 0)[1], 0, unroll=unroll)

        return 0

    lax.fori_loop(0, units, unit, 0)


def stats_kernel(rows, pieces, row_max, row_sum, stats_out):
    lane = lax.broadcasted_iota(jnp.int32, (rows, LANES), 1)
    stats = jnp.zeros((rows, LANES), jnp.float32)
    for t in range(pieces):
        for k in range(4):
            start = (4 * t + k) * rows
            at = slice(start, start + rows)
            total = jnp.sum(row_sum[at, :], axis=1, keepdims=True)
            stats = jnp.where(lane == 8 * t + k, row_max[at, :], stats)
            stats = jnp.where(lane == 8 * t + 4 + k, total, stats)
    stats_out[...] = stats.T[: 8 * pieces, :]


def stats_of(row_max, row_sum, pieces):
    rows = row_max.shape[0] // (4 * pieces)
    vmem = pl.BlockSpec(memory_space=pltpu.VMEM)
    return pl.pallas_call(
        functools.partial(stats_kernel, rows, pieces),
        out_shape=jax.ShapeDtypeStruct((8 * pieces, rows), jnp.float32),
        in_specs=[vmem] * 2,
        out_specs=vmem,
        compiler_params=pltpu.CompilerParams(vmem_limit_bytes=KERNEL_VMEM),
        name="stats",
    )(row_max, row_sum)


def fold_planes(place, flags, queries, pairs, state, pieces):
    first = state is None
    units = len(pairs)
    keys_here, width = sum(x.shape[0] for x in pairs[0]), pairs[0][0].shape[1]
    rows = keys_here // 2
    chunks = [x for pair in pairs for x in pair]
    vmem = pl.BlockSpec(memory_space=pltpu.VMEM)
    smem = pl.BlockSpec(memory_space=pltpu.SMEM)
    all_rows = pieces * 4 * rows
    state_shapes = [
        jax.ShapeDtypeStruct((all_rows, VAL_DIM), jnp.float32),
        jax.ShapeDtypeStruct((all_rows, LANES), jnp.float32),
        jax.ShapeDtypeStruct((all_rows, LANES), jnp.float32),
    ]
    if first:
        operands = [place, flags, *queries, *chunks]
        out_shape = [jax.ShapeDtypeStruct((all_rows, HEAD_DIM), jnp.bfloat16), *state_shapes]
        aliases = {}
    else:
        operands = [place, flags, queries, *chunks, *state]
        out_shape = list(state_shapes)
        aliases = {3 + units + i: i for i in range(3)}
    terms = all_rows * keys_here * units
    return pl.pallas_call(
        functools.partial(fold_kernel, first, units, rows, pieces),
        out_shape=out_shape,
        in_specs=[smem, smem] + [vmem] * (len(operands) - 2),
        out_specs=[vmem] * len(out_shape),
        scratch_shapes=[pltpu.VMEM((units, keys_here, width), jnp.bfloat16)],
        input_output_aliases=aliases,
        compiler_params=pltpu.CompilerParams(vmem_limit_bytes=KERNEL_VMEM),
        cost_estimate=pl.CostEstimate(
            flops=2 * terms * (HEAD_DIM + VAL_DIM), transcendentals=terms, bytes_accessed=0
        ),
        name="planes_first" if first else "planes",
    )(*operands)


def difference_kernel(rows, pieces, lambdas, acc, *refs):
    stats, (own, *outs) = refs[:pieces], refs[pieces:]
    coefs = []
    for t in range(pieces):
        tiles = []
        for s in range(pieces):
            at = 8 * ((t - s) % pieces)
            tiles.append(stats[s][at : at + 8, :])
        top = functools.reduce(jnp.maximum, tiles)
        total = jnp.zeros_like(top)
        for s in range(pieces):
            share = jnp.exp2((tiles[s] - top) * EXP2_SCALE)
            if s == 0:
                own_share = share
            total = total + share * jnp.concatenate([tiles[s][4:], tiles[s][:4]], axis=0)
        coefs.append(own_share / total)
    coefs.append(jnp.zeros((LANES - 8 * pieces, rows), jnp.float32))
    coefs = jnp.concatenate(coefs, axis=0).T
    for t, out in enumerate((own, *outs)):
        for h in range(2):
            start = t * 4 * rows + h * rows
            one, two = 8 * t + h, 8 * t + 2 + h
            mix_one = acc[start : start + rows, :] * coefs[:, one : one + 1]
            start += 2 * rows
            mix_two = acc[start : start + rows, :] * coefs[:, two : two + 1]
            out[h * rows : (h + 1) * rows, :] = (mix_one - lambdas[h] * mix_two).astype(out.dtype)


def differences(lambdas, acc, stats):
    pieces = len(stats)
    rows = acc.shape[0] // (4 * pieces)
    vmem = pl.BlockSpec(memory_space=pltpu.VMEM)
    shape = (2 * rows, VAL_DIM)
    return pl.pallas_call(
        functools.partial(difference_kernel, rows, pieces),
        out_shape=[jax.ShapeDtypeStruct(shape, jnp.float32)]
        + [jax.ShapeDtypeStruct(shape, jnp.bfloat16)] * (pieces - 1),
        in_specs=[pl.BlockSpec(memory_space=pltpu.SMEM)] + [vmem] * (1 + pieces),
        out_specs=[vmem] * pieces,
        compiler_params=pltpu.CompilerParams(vmem_limit_bytes=KERNEL_VMEM),
        cost_estimate=pl.CostEstimate(
            flops=3 * acc.size, transcendentals=0, bytes_accessed=4 * acc.size
        ),
        name="differences",
    )(lambdas, acc, *stats)


def project_kernel(rows, gain, weight, own, *refs):
    shares, out = refs[:-1], refs[-1]
    heads = []
    for h in range(2):
        at = slice(h * rows, (h + 1) * rows)
        difference = own[at, :]
        for share in shares:
            difference = difference + share[at, :].astype(jnp.float32)
        mean_sq = jnp.mean(difference * difference, axis=-1, keepdims=True)
        normed = difference * lax.rsqrt(mean_sq + EPS) * gain[...] * OUT_SCALE
        heads.append(normed.astype(jnp.bfloat16))
    heads_out = jnp.concatenate(heads, axis=1)
    out[...] = jnp.dot(heads_out, weight[...], preferred_element_type=jnp.float32).astype(
        jnp.bfloat16
    )


def project(head_gain, out_weight, own, shares):
    rows = own.shape[0] // 2
    vmem = pl.BlockSpec(memory_space=pltpu.VMEM)
    return pl.pallas_call(
        functools.partial(project_kernel, rows),
        out_shape=jax.ShapeDtypeStruct((rows, out_weight.shape[1]), jnp.bfloat16),
        in_specs=[vmem] * (3 + len(shares)),
        out_specs=vmem,
        compiler_params=pltpu.CompilerParams(vmem_limit_bytes=KERNEL_VMEM),
        cost_estimate=pl.CostEstimate(
            flops=2 * rows * out_weight.size, transcendentals=0, bytes_accessed=out_weight.size * 2
        ),
        name="project",
    )(head_gain.reshape(1, -1), out_weight, own, *shares)


def run_copies(moves, sems):
    copies = [
        pltpu.make_async_copy(source, target, sems.at[i])
        for i, (source, target) in enumerate(moves)
    ]
    for copy in copies:
        copy.start()
    for copy in copies:
        copy.wait()


def pack_kernel(key_one, key_two, values, query_one, query_two, keys_out, queries_out, sems):
    d, width = HEAD_DIM, query_one.shape[1]
    run_copies(
        [
            (key_one, keys_out.at[:, :d]),
            (key_two, keys_out.at[:, d : 2 * d]),
            (values, keys_out.at[:, 2 * d :]),
            (query_one, queries_out.at[:, :width]),
            (query_two, queries_out.at[:, width:]),
        ],
        sems,
    )


def pack(keys_one, keys_two, values, queries_one, queries_two):
    rows = values.shape[0]
    vmem = pl.BlockSpec(memory_space=pltpu.VMEM)
    width = 2 * HEAD_DIM + VAL_DIM
    return pl.pallas_call(
        pack_kernel,
        out_shape=[jax.ShapeDtypeStruct((rows, width), jnp.bfloat16)] * 2,
        in_specs=[pl.BlockSpec(memory_space=pltpu.HBM)] * 5,
        out_specs=[vmem] * 2,
        scratch_shapes=[pltpu.SemaphoreType.DMA((5,))],
        compiler_params=pltpu.CompilerParams(vmem_limit_bytes=PACK_VMEM),
        name="pack",
    )(keys_one, keys_two, values, queries_one, queries_two)


def pack_weights_kernel(gate, up, down, low_out, high_out, low, high, sems):
    width, units = gate.shape[1:]
    half = width // 2
    blocks = width // units

    def copy(source, target, i):
        return pltpu.make_async_copy(source, target, sems.at[i])

    to_low = [copy(gate.at[0], low.at[:width], 0), copy(up.at[0, :half], low.at[width:], 1)]
    to_high = [copy(up.at[0, half:], high.at[:half], 2)]
    for j in range(blocks):
        at = half + j * units
        columns = down.at[0, :, j * units : (j + 1) * units]
        to_high.append(copy(columns, high.at[at : at + units], 3 + j))
    out_low, out_high = copy(low, low_out, 3 + blocks), copy(high, high_out, 4 + blocks)
    for move in to_low + to_high:
        move.start()
    for move in to_low:
        move.wait()
    out_low.start()
    for move in to_high:
        move.wait()
    out_high.start()
    out_low.wait()
    out_high.wait()


def pack_weights(gate, up, down):
    width, units = gate.shape[1:]
    hbm = pl.BlockSpec(memory_space=pltpu.HBM)
    return pl.pallas_call(
        pack_weights_kernel,
        out_shape=[jax.ShapeDtypeStruct((width + width // 2, units), gate.dtype)] * 2,
        in_specs=[hbm] * 3,
        out_specs=[hbm] * 2,
        scratch_shapes=[pltpu.VMEM((width + width // 2, units), gate.dtype)] * 2
        + [pltpu.SemaphoreType.DMA((5 + width // units,))],
        compiler_params=pltpu.CompilerParams(vmem_limit_bytes=ALL_VMEM),
        name="pack_weights",
    )(gate, up, down)


def places():
    planes = lax.axis_size("z")
    plane, y, core = lax.axis_index("z"), lax.axis_index("y"), lax.axis_index("core")
    half = planes // 2

    def held(d, from_below):
        return jnp.where(from_below, plane - d, plane + d - planes)

    flags = [jnp.stack([plane, held(1, core == 0)])]
    for d in range(2, half + 1):
        reached = held(d, core == 0) if d < half else plane - d
        flags.append(jnp.stack([reached, held(d - 1, core == 1)]))
    flags = [(flag >= 0).astype(jnp.int32) for flag in flags]
    return jnp.stack([y, core]).astype(jnp.int32), flags


def attend(place, flags, queries_one, queries_two, keys_one, keys_two, values, lambdas):
    planes, pieces = lax.axis_size("z"), lax.axis_size("y")
    swap = [(0, 1), (1, 0)]
    packed, both = pack(keys_one, keys_two, values, queries_one, queries_two)
    queries = [both]
    for t in range(1, pieces):
        queries.append(lax.ppermute(both, "y", [(i, (i + t) % pieces) for i in range(pieces)]))
    partner = lax.ppermute(packed, "core", swap)

    half = planes // 2
    received, swapped = [None], [None]
    for d in range(1, half + 1):
        moves = [((z - 1, 0), (z, 0)) for z in range(d, planes)]
        for first_plane in range(half):
            z = (first_plane - d) % planes
            moves.append((((z + 1) % planes, 1), (z, 1)))

        def along(x, flip):
            flat = [(2 * a + (b ^ flip), 2 * e + f) for (a, b), (e, f) in moves]
            return lax.ppermute(x, ("z", "core"), flat)

        if d == 1:
            received.append(jnp.concatenate([along(packed, 0), along(packed, 1)], 0))
        else:
            received.append(along(received[-1], 0))
        if d < half:
            swapped.append(lax.ppermute(received[-1], "core", swap))

    q_all, *state = fold_planes(
        place, flags[0], queries, [(packed, partner), (received[1],)], None, pieces
    )
    for d in range(2, half + 1):
        pairs = [(received[d],), (swapped[d - 1],)]
        state = fold_planes(place, flags[d - 1], q_all, pairs, state, pieces)
    acc, row_max, row_sum = state
    own_stats = stats_of(row_max, row_sum, pieces)
    stats = [own_stats]
    for t in range(1, pieces):
        ring = [(i, (i + t) % pieces) for i in range(pieces)]
        stats.append(lax.ppermute(own_stats, "y", ring))
    own, *others = differences(lambdas, acc, stats)
    shares = []
    for t in range(1, pieces):
        ring = [(i, (i - t) % pieces) for i in range(pieces)]
        shares.append(lax.ppermute(others[t - 1], "y", ring))
    return own, shares


def dispatch_kernel(tiles, stream_in, gain, selector, stream_out, send):
    attended = tiles[0].astype(jnp.float32)
    for t in range(1, tiles.shape[0]):
        attended = attended + tiles[t].astype(jnp.float32)
    stream = stream_in[...].astype(jnp.float32) + attended
    stream_out[...] = stream
    mean_sq = jnp.mean(stream * stream, axis=-1, keepdims=True)
    normed = (stream * lax.rsqrt(mean_sq + EPS) * gain[...]).astype(jnp.bfloat16)
    send[...] = jnp.dot(selector[...], normed, preferred_element_type=jnp.float32).astype(
        jnp.bfloat16
    )


def dispatch(tiles, stream_in, norm_gain, selector):
    rows, width = stream_in.shape
    vmem = pl.BlockSpec(memory_space=pltpu.VMEM)
    return pl.pallas_call(
        dispatch_kernel,
        out_shape=[
            jax.ShapeDtypeStruct((rows, width), jnp.float32),
            jax.ShapeDtypeStruct((selector.shape[0], width), jnp.bfloat16),
        ],
        in_specs=[vmem] * 4,
        out_specs=[vmem] * 2,
        compiler_params=pltpu.CompilerParams(vmem_limit_bytes=KERNEL_VMEM),
        cost_estimate=pl.CostEstimate(
            flops=2 * selector.size * width, transcendentals=0, bytes_accessed=4 * tiles.size
        ),
        name="dispatch",
    )(tiles, stream_in, norm_gain.reshape(1, -1), selector)


def experts_kernel(rows_in, *refs):
    sources, (out, held, sums, sems) = refs[:8], refs[8:]
    width, units = rows_in.shape[1], held.shape[2]
    half = width // 2

    def moves(g, low, high):
        return [
            pltpu.make_async_copy(low, held.at[g, : width + half], sems.at[g, 0]),
            pltpu.make_async_copy(
                high.at[:half], held.at[g, width + half : 2 * width], sems.at[g, 1]
            ),
            pltpu.make_async_copy(high.at[half:], held.at[g, 2 * width :], sems.at[g, 2]),
        ]

    def start(g):
        for move in moves(g, *sources[2 * g : 2 * g + 2]):
            move.start()

    start(0)
    start(1)
    sums[...] = jnp.zeros_like(sums)

    def add_group(g, _):
        for ahead in (2, 3):
            pl.when(g == ahead - 2)(functools.partial(start, ahead))
        waits = moves(g, *sources[:2])
        waits[0].wait()
        waits[1].wait()
        picked = rows_in[...]
        gated = jnp.dot(picked, held[g, :width], preferred_element_type=jnp.float32)
        upper = jnp.dot(picked, held[g, width : 2 * width], preferred_element_type=jnp.float32)
        hidden = (gated / (1.0 + jnp.exp(-gated)) * upper).astype(jnp.bfloat16)
        waits[2].wait()
        for j in range(0, width, units):
            sums[:, j : j + units] += jnp.dot(
                hidden,
                held[g, 2 * width + j : 2 * width + j + units],
                preferred_element_type=jnp.float32,
            )
        return 0

    lax.fori_loop(0, 4, add_group, 0)
    out[...] = sums[...].astype(jnp.bfloat16)


def experts(rows_in, weights):
    rows, width = rows_in.shape
    units = weights[0].shape[1]
    vmem = pl.BlockSpec(memory_space=pltpu.VMEM)
    return pl.pallas_call(
        experts_kernel,
        out_shape=jax.ShapeDtypeStruct((rows, width), jnp.bfloat16),
        in_specs=[vmem] + [pl.BlockSpec(memory_space=pltpu.HBM)] * 8,
        out_specs=vmem,
        scratch_shapes=[
            pltpu.VMEM((4, 3 * width, units), jnp.bfloat16),
            pltpu.VMEM((rows, width), jnp.float32),
            pltpu.SemaphoreType.DMA((4, 3)),
        ],
        compiler_params=pltpu.CompilerParams(vmem_limit_bytes=EXPERTS_VMEM),
        cost_estimate=pl.CostEstimate(
            flops=24 * rows * width * units, transcendentals=4 * rows * units, bytes_accessed=24 * width * units
        ),
        name="experts",
    )(rows_in, *weights)


def collect_kernel(returned, choice_one, choice_two, route_weight, stream, out):
    picked_one = jnp.dot(choice_one[...], returned[...], preferred_element_type=jnp.float32)
    picked_two = jnp.dot(choice_two[...], returned[...], preferred_element_type=jnp.float32)
    routed = picked_one * route_weight[:, 0:1] + picked_two * route_weight[:, 1:2]
    out[...] = (stream[...] + routed).astype(jnp.bfloat16)


def collect(returned, choice_one, choice_two, route_weight, stream):
    vmem = pl.BlockSpec(memory_space=pltpu.VMEM)
    return pl.pallas_call(
        collect_kernel,
        out_shape=jax.ShapeDtypeStruct(stream.shape, jnp.bfloat16),
        in_specs=[vmem] * 5,
        out_specs=vmem,
        compiler_params=pltpu.CompilerParams(vmem_limit_bytes=KERNEL_VMEM),
        cost_estimate=pl.CostEstimate(
            flops=4 * choice_one.size * stream.shape[1], transcendentals=0, bytes_accessed=2 * returned.size
        ),
        name="collect",
    )(returned, choice_one, choice_two, route_weight, stream)


def body(
    stream_in,
    queries_one,
    queries_two,
    keys_one,
    keys_two,
    values,
    lambdas,
    head_gain,
    out_weight,
    norm_gain,
    expert_ids,
    route_weight,
    gate_weight,
    up_weight,
    down_weight,
):
    peers = lax.axis_size("tp")

    up_ring = [(i, (i + 1) % peers) for i in range(peers)]
    down_ring = [(i, (i - 1) % peers) for i in range(peers)]
    own_low, own_high = pack_weights(gate_weight, up_weight, down_weight)
    below = [lax.ppermute(w, "tp", up_ring) for w in (own_low, own_high)]
    above = [lax.ppermute(w, "tp", down_ring) for w in (own_low, own_high)]
    across = [lax.ppermute(below[0], "tp", up_ring), lax.ppermute(above[1], "tp", down_ring)]
    weights = [own_low, own_high, *below, *above, *across]

    rows_here = stream_in.shape[0]
    top_count = expert_ids.shape[1]
    experts_all = lax.axis_size(SP_AXES)
    slot_cap = 2 * top_count * rows_here // experts_all
    flat_ids = expert_ids.reshape(-1)
    one_hot = (flat_ids[:, None] == lax.iota(jnp.int32, experts_all)[None, :]).astype(jnp.int32)
    ranks = jnp.sum((jnp.cumsum(one_hot, axis=0) - 1) * one_hot, axis=1)
    slots = (flat_ids * slot_cap + ranks).reshape(rows_here, top_count)
    all_slots = lax.iota(jnp.int32, experts_all * slot_cap)
    choice_one = (slots[:, 0:1] == all_slots[None, :]).astype(jnp.bfloat16)
    choice_two = (slots[:, 1:2] == all_slots[None, :]).astype(jnp.bfloat16)
    selector = (choice_one + choice_two).T

    place, flags = places()
    route_weight = jnp.pad(route_weight, ((0, 0), (0, LANES - top_count)))
    place, flags, choice_one, choice_two, selector, route_weight = lax.optimization_barrier(
        (place, flags, choice_one, choice_two, selector, route_weight)
    )
    own, shares = attend(
        place, flags, queries_one, queries_two, keys_one, keys_two, values, lambdas
    )
    partial_rows = project(head_gain, out_weight, own, shares)
    tiles = lax.all_to_all(
        partial_rows.reshape(peers, rows_here, -1), "tp", 0, 0, tiled=True
    )
    stream, send_rows = dispatch(tiles, stream_in, norm_gain, selector)
    received = lax.all_to_all(
        send_rows, SP_AXES, split_axis=0, concat_axis=0, tiled=True
    )
    results = experts(received, weights)
    returned = lax.all_to_all(results, SP_AXES, split_axis=0, concat_axis=0, tiled=True)
    return collect(returned, choice_one, choice_two, route_weight, stream)


def solution(mesh):
    sp, tp = mesh.devices.shape
    planes = max(sp // 8, 2)
    split = Mesh(
        mesh.devices.reshape(planes, sp // (2 * planes), 2, tp), ("z", "y", "core", "tp")
    )
    everywhere = ("z", "y", "core", "tp")
    sp_axes = SP_AXES
    return jax.shard_map(
        body,
        mesh=split,
        in_specs=(
            P(everywhere, None),
            P(sp_axes, "tp"),
            P(sp_axes, "tp"),
            P(sp_axes, "tp"),
            P(sp_axes, "tp"),
            P(sp_axes, "tp"),
            P("tp"),
            P(),
            P("tp", None),
            P(),
            P(everywhere, None),
            P(everywhere, None),
            P(sp_axes, None, "tp"),
            P(sp_axes, None, "tp"),
            P(sp_axes, "tp", None),
        ),
        out_specs=P(everywhere, None),
        check_vma=False,
    )
```
